512 devices in a mesh: ep: 128 (over z, x, core), tp: 4 (over y).
Axes of the slice: x: 4, y: 4, z: 16, core: 2. Of those that a mesh axis runs over, the one named last changes fastest.
Arguments:
- tokens: bfloat16 [2048, 2048], P('ep', 'tp'), may hold values from -6 to 6
- state: bfloat16 [2048, 32, 4096], P('ep', 'tp'), may hold values from -6 to 6
- mix_gain: float32 [2048], P('tp'), may hold values from 0.1 to 1.9
- w_recept: bfloat16 [2048, 2048], P('tp', 'ep'), may hold values from -0.125 to 0.125
- w_key: bfloat16 [2048, 2048], P('tp', 'ep'), may hold values from -0.125 to 0.125
- w_value: bfloat16 [2048, 2048], P('tp', 'ep'), may hold values from -0.125 to 0.125
- w_decay: bfloat16 [2048, 2048], P('tp', 'ep'), may hold values from -0.125 to 0.125
- w_rate: bfloat16 [2048, 2048], P('tp', 'ep'), may hold values from -0.125 to 0.125
- decay_base: float32 [2048], P('tp'), may hold values from -4 to 2
- rate_base: float32 [2048], P('tp'), may hold values from -2 to 2
- head_gain: float32 [2048], P('tp'), may hold values from 0.1 to 1.9
- w_out: bfloat16 [2048, 2048], P('tp', 'ep'), may hold values from -0.125 to 0.125
- moe_gain: float32 [2048], replicated, may hold values from 0.1 to 1.9
- routes: int32 [2048, 6], P('ep'), may hold values from 0 to 127, all different within a row; in each aligned block of 16 rows (0 to 15, 16 to 31, ...) at most 2 rows name the same one
- route_weight: float32 [2048, 6], P('ep'), may hold values from 0.1 to 1
- expert_gate: bfloat16 [128, 2048, 512], P('ep', None, 'tp'), may hold values from -0.125 to 0.125
- expert_up: bfloat16 [128, 2048, 512], P('ep', None, 'tp'), may hold values from -0.125 to 0.125
- expert_down: bfloat16 [128, 512, 2048], P('ep', 'tp'), may hold values from -0.25 to 0.25
- shared_gate: bfloat16 [2048, 512], P(None, 'tp'), may hold values from -0.125 to 0.125
- shared_up: bfloat16 [2048, 512], P(None, 'tp'), may hold values from -0.125 to 0.125
- shared_down: bfloat16 [512, 2048], P('tp'), may hold values from -0.25 to 0.25
Outputs:
- layer_out: bfloat16 [2048, 2048], P('ep', 'tp')
The draws below stay inside these ranges and needn't reach their ends.
Inputs may be any that keep to these rules, and one draw needn't show every extreme that they name: `routes`: each row names 6 different experts. Within the rows of one device (aligned blocks of 16 rows) no expert is named by more than 2 rows, a bound that some block reaches.
All inputs are finite; a program needn't handle non-finite values.
Results may differ from the reference program's by a relative error of at most 0.024.
Values may be sent and summed in bfloat16 or wider, within the bound.
A program may use at most 64 MiB of HBM per device.

```python
import math
import jax
import jax.numpy as jnp
import numpy as np
from jax import lax

D = 2048
HEADS = 32
HEAD = 64
F = 512
FS = 512
TOPK = 6
SEQ_DEV = 16
TOKENS = 2048
EXPERTS = 128
CAP = 2
DA = 2048
N_EP = 128
N_TP = 4


def shard_levels(stream_key, shape, split, smallest, top_value):
    gain, own = 1.0, jax.random.fold_in(stream_key, 6)
    for dim, parts in split:
        heights = jnp.exp(jax.random.uniform(jax.random.fold_in(own, dim), (parts,), jnp.float32, smallest / len(split), top_value / len(split)))
        gain = gain * jnp.repeat(heights, shape[dim] // parts).reshape([-1 if axis == dim else 1 for axis in range(len(shape))])
    return gain


def deal_out(own_key, own, number, rows, number_of, top, bound, slope):
    ranking = jax.random.permutation(own_key, number_of)
    packed, usual = portions_of(number_of, rows * top, bound, slope, True), portions_of(number_of, rows * top, bound, slope, False)
    places = jnp.arange(number_of)

    def named(lengths, offset_by):
        used = int((lengths > 0).sum())
        fixed = max(1, used // 4)
        shifted = fixed + (places - fixed + offset_by * (used - fixed)) % max(1, number_of - fixed)
        return jnp.zeros((number_of,), jnp.int32).at[ranking[jnp.where(places < fixed, places, shifted)]].set(jnp.asarray(lengths, jnp.int32))

    lengths = jnp.where(number % 4 == 0, named(packed, number // 4), named(usual, number - number // 4 - 1))
    mixed = jax.random.permutation(jax.random.fold_in(own, 3), number_of)
    giver, sink = mixed[0:number_of // 2 * 2:2], mixed[1:number_of // 2 * 2:2]
    slack = jnp.minimum(lengths[giver] - 1, bound - lengths[sink]) // 2
    slack = jnp.where((giver == ranking[0]) | (sink == ranking[0]) | (lengths[sink] == 0), 0, jnp.maximum(slack, 0))
    shifted = jax.random.randint(jax.random.fold_in(own, 4), (number_of // 2,), 0, 1 << 20) % (slack + 1)
    lengths = lengths.at[giver].add(-shifted).at[sink].add(shifted)
    items = jnp.searchsorted(jnp.cumsum(lengths), jnp.arange(rows * top), side="right").astype(jnp.int32)
    table = items.reshape(top, rows).T
    table = table[jax.random.permutation(jax.random.fold_in(own, 1), rows)]
    offset_by = jax.random.randint(jax.random.fold_in(own, 2), (rows, 1), 0, top)
    return jnp.take_along_axis(table, (jnp.arange(top)[None, :] + offset_by) % top, axis=1)


def portions_of(count, total, most, lean, full):
    portions = [(1 << 20) // math.isqrt(grade ** lean) + 1 for grade in range(1, count + 1)]
    largest = most if full else min(most, max(-(-total // count), total * portions[0] // sum(portions)))
    least = 1 if total - largest >= count - 1 else 0
    counts, surplus = [largest] + [least] * (count - 1), total - largest - least * (count - 1)
    while surplus > 0:
        candidates = [i for i in range(1, count) if counts[i] < largest] or [i for i in range(1, count) if counts[i] < most]
        mass, left = sum([portions[i] for i in candidates]), surplus
        for i in candidates:
            more = min(most - counts[i], max(1, left * portions[i] // mass), surplus)
            counts[i] = counts[i] + more
            surplus = surplus - more
    return np.array(counts)


def gaussian(rng, shape, width, bound, shards=(), kind=jnp.bfloat16):
    drawn = width * jax.random.normal(rng, shape, jnp.float32)
    if shards:
        drawn = drawn * shard_levels(rng, shape, shards, -0.22, 0.18)
    return jnp.clip(drawn, -bound, bound).astype(kind)


def setup_inputs(seed: int = 0) -> dict:
    splits = jax.random.split(jax.random.key(seed), 22)
    tokens = gaussian(splits[0], (TOKENS, D), 1.0, 6.0, ((0, 128), (1, 4)))
    state = gaussian(splits[1], (TOKENS, HEADS, HEAD * HEAD), 1.0, 6.0, ((0, 128), (1, 4)))
    mix_gain = jnp.clip(1.0 + 0.18 * jax.random.normal(splits[2], (D,), jnp.float32), 0.1, 1.9)
    w_recept = gaussian(splits[3], (D, DA), D ** -0.5, 0.125, ((0, 4), (1, 128)))
    w_key = gaussian(splits[4], (D, DA), D ** -0.5, 0.125, ((0, 4), (1, 128)))
    w_value = gaussian(splits[5], (D, DA), D ** -0.5, 0.125, ((0, 4), (1, 128)))
    w_decay = gaussian(splits[6], (D, DA), D ** -0.5, 0.125, ((0, 4), (1, 128)))
    w_rate = gaussian(splits[7], (D, DA), D ** -0.5, 0.125, ((0, 4), (1, 128)))
    decay_base = jnp.clip(-4.0 + 6.0 * jax.random.uniform(splits[8], (DA,), jnp.float32) ** shard_levels(splits[8], (DA,), ((0, 4),), -0.2, 0.2), -4.0, 2.0)
    rate_base = jnp.clip(jax.random.uniform(splits[9], (DA,), jnp.float32, -2.0, 2.0) * shard_levels(splits[9], (DA,), ((0, 4),), -0.4, 0.0), -2.0, 2.0)
    head_gain = jnp.clip(1.0 + 0.18 * jax.random.normal(splits[10], (DA,), jnp.float32), 0.1, 1.9)
    w_out = gaussian(splits[11], (DA, D), DA ** -0.5, 0.125, ((0, 4), (1, 128)))
    moe_gain = jnp.clip(1.0 + 0.18 * jax.random.normal(splits[12], (D,), jnp.float32), 0.1, 1.9)
    routes_keys = jax.random.split(jax.random.fold_in(splits[13], 1), TOKENS // SEQ_DEV)
    routes_turns = jax.random.permutation(jax.random.fold_in(splits[13], 3), TOKENS // SEQ_DEV)
    routes = jax.vmap(lambda own, number: deal_out(jax.random.fold_in(splits[13], 2), own, number, SEQ_DEV, EXPERTS, TOPK, CAP, 2))(routes_keys, routes_turns).reshape((TOKENS, TOPK))
    route_weight = jnp.clip(jnp.exp(math.log(1.0) - 2.3025851 * jax.random.uniform(splits[14], (TOKENS, TOPK), jnp.float32) ** shard_levels(splits[14], (TOKENS, TOPK), ((0, 128),), -0.2, 0.2)), 0.1, 1.0)
    expert_gate = gaussian(splits[15], (EXPERTS, D, F), D ** -0.5, 0.125, ((0, 128), (2, 4)))
    expert_up = gaussian(splits[16], (EXPERTS, D, F), D ** -0.5, 0.125, ((0, 128), (2, 4)))
    expert_down = gaussian(splits[17], (EXPERTS, F, D), F ** -0.5, 0.25, ((0, 128), (1, 4)))
    shared_gate = gaussian(splits[18], (D, FS), D ** -0.5, 0.125, ((1, 4),))
    shared_up = gaussian(splits[19], (D, FS), D ** -0.5, 0.125, ((1, 4),))
    shared_down = gaussian(splits[20], (FS, D), FS ** -0.5, 0.25, ((0, 4),))
    return dict(tokens=tokens, state=state, mix_gain=mix_gain, w_recept=w_recept, w_key=w_key, w_value=w_value, w_decay=w_decay, w_rate=w_rate, decay_base=decay_base, rate_base=rate_base, head_gain=head_gain, w_out=w_out, moe_gain=moe_gain, routes=routes, route_weight=route_weight, expert_gate=expert_gate, expert_up=expert_up, expert_down=expert_down, shared_gate=shared_gate, shared_up=shared_up, shared_down=shared_down)


RMS_EPS = 1e-06
GN_EPS = 0.00064
KEY_EPS = 1e-06
ROUTED_SCALE = 2.5

def row_norm(row_vals, gain_vals):
    row32 = row_vals.astype(jnp.float32)
    factor = lax.rsqrt(lax.optimization_barrier(jnp.mean(row32 * row32, axis=-1, keepdims=True)) + RMS_EPS)
    return (row32 * factor * gain_vals).astype(jnp.bfloat16)

def quarter_dot(left_vals, weight):
    row_count = left_vals.shape[0]
    part_len = left_vals.shape[1] // N_TP
    left_parts = left_vals.reshape(row_count, N_TP, part_len).astype(jnp.float32)
    weight_parts = weight.reshape(N_TP, part_len, weight.shape[1]).astype(jnp.float32)
    partial_value = jnp.einsum('rqk,qkm->rqm', left_parts, weight_parts)
    rounded = lax.optimization_barrier(partial_value.astype(jnp.bfloat16))
    return lax.optimization_barrier(jnp.sum(rounded.astype(jnp.float32), axis=1))

def mixer_rows(state_rows, projected, decay_base, rate_base, head_gain):
    seq_count = projected.shape[0]
    head_count = projected.shape[2] // HEAD

    def per_head(column):
        return projected[:, column, :].reshape(seq_count, head_count, HEAD)
    receptance = per_head(0)
    key_vec = per_head(1)
    value_vec = per_head(2)
    decay_pre = (projected[:, 3, :] + decay_base).reshape(seq_count, head_count, HEAD)
    rate_pre = (projected[:, 4, :] + rate_base).reshape(seq_count, head_count, HEAD)
    decay_rate = jnp.exp(-jnp.exp(-jax.nn.softplus(-decay_pre) - 0.5))
    in_rate = jax.nn.sigmoid(rate_pre)
    unit_key = key_vec * lax.rsqrt(lax.optimization_barrier(jnp.sum(key_vec * key_vec, axis=-1, keepdims=True)) + KEY_EPS)
    carried = state_rows.astype(jnp.float32).reshape(seq_count, head_count, HEAD, HEAD)
    removed = jnp.einsum('nhvk,nhk->nhv', carried, unit_key)
    updated = carried * decay_rate[:, :, None, :] - removed[:, :, :, None] * (unit_key * in_rate)[:, :, None, :] + value_vec[:, :, :, None] * (key_vec * in_rate)[:, :, None, :]
    readout = jnp.einsum('nhvk,nhk->nhv', updated, receptance)
    centre = lax.optimization_barrier(jnp.mean(readout, axis=-1, keepdims=True))
    spread = lax.optimization_barrier(jnp.mean(jnp.square(readout - centre), axis=-1, keepdims=True))
    normed = (readout - centre) * lax.rsqrt(spread + GN_EPS)
    return (normed.reshape(seq_count, head_count * HEAD) * head_gain).astype(jnp.bfloat16)

def reference(tokens, state, mix_gain, w_recept, w_key, w_value, w_decay, w_rate, decay_base, rate_base, head_gain, w_out, moe_gain, routes, route_weight, expert_gate, expert_up, expert_down, shared_gate, shared_up, shared_down):
    normed = row_norm(tokens, mix_gain)
    projected = jnp.stack([quarter_dot(normed, weight) for weight in (w_recept, w_key, w_value, w_decay, w_rate)], axis=1)

    def mix_group(item):
        return mixer_rows(item[0], item[1], decay_base, rate_base, head_gain)
    mixed = lax.map(mix_group, (state.reshape(N_EP, SEQ_DEV, HEADS, HEAD * HEAD), projected.reshape(N_EP, SEQ_DEV, 5, HEADS * HEAD)))
    mixed = mixed.reshape(TOKENS, HEADS * HEAD)
    attended = quarter_dot(mixed, w_out)
    resid = (tokens.astype(jnp.float32) + attended).astype(jnp.bfloat16)
    normed_two = row_norm(resid, moe_gain)
    shared_hidden = (jax.nn.silu(jnp.dot(normed_two, shared_gate, preferred_element_type=jnp.float32)) * jnp.dot(normed_two, shared_up, preferred_element_type=jnp.float32)).astype(jnp.bfloat16)
    shared_out = quarter_dot(shared_hidden, shared_down)
    per_group = SEQ_DEV * TOPK
    grouped = routes.reshape(N_EP, per_group)
    position = jnp.arange(per_group, dtype=jnp.int32)
    earlier = (grouped[:, :, None] == grouped[:, None, :]) & (position[None, None, :] < position[None, :, None])
    rank_in = lax.optimization_barrier(jnp.sum(earlier.astype(jnp.int32), axis=2))
    group_ids = jnp.arange(N_EP, dtype=jnp.int32)[:, None]
    flat_slot = ((grouped * N_EP + group_ids) * CAP + rank_in).reshape(-1).astype(jnp.int32)
    owner_token = (jnp.arange(TOKENS, dtype=jnp.int32)[:, None] + jnp.zeros((1, TOPK), jnp.int32)).reshape(-1)
    slot_total = EXPERTS * N_EP * CAP
    table = jnp.zeros((slot_total,), jnp.int32).at[flat_slot].set(owner_token)
    live = jnp.zeros((slot_total,), jnp.float32).at[flat_slot].set(1.0)

    def run_expert(item):
        row_index, live_rows, gate_w, up_w, down_w = item
        chosen_rows = jnp.take(normed_two, row_index, axis=0)
        gate_val = jnp.dot(chosen_rows, gate_w, preferred_element_type=jnp.float32)
        up_val = jnp.dot(chosen_rows, up_w, preferred_element_type=jnp.float32)
        hidden = (jax.nn.silu(gate_val) * up_val).astype(jnp.bfloat16)
        return (quarter_dot(hidden, down_w) * live_rows[:, None]).astype(jnp.bfloat16)
    expert_rows = lax.map(run_expert, (table.reshape(EXPERTS, N_EP * CAP), live.reshape(EXPERTS, N_EP * CAP), expert_gate, expert_up, expert_down))
    picked = jnp.take(expert_rows.reshape(slot_total, D), flat_slot, axis=0)
    picked = picked.astype(jnp.float32).reshape(TOKENS, TOPK, D)
    share = route_weight / lax.optimization_barrier(jnp.sum(route_weight, axis=1, keepdims=True)) * ROUTED_SCALE
    routed = lax.optimization_barrier(jnp.sum(share[:, :, None] * picked, axis=1))
    return (resid.astype(jnp.float32) + routed + shared_out).astype(jnp.bfloat16)
```

```python
import functools

import jax
import jax.numpy as jnp
from jax import lax
from jax.experimental import pallas as pl
from jax.experimental.pallas import tpu as pltpu
from jax.sharding import Mesh
from jax.sharding import PartitionSpec as P

HEAD = 64
LANES = 128
RMS_EPS = 1e-06
GN_EPS = 0.00064
KEY_EPS = 1e-06
ROUTED_SCALE = 2.5
AXES = ("ep_0", "ep_1", "ep_2", "tp")
EP = AXES[:3]
MESH_ID = pl.DeviceIdType.MESH
F32 = jnp.float32
BF16 = jnp.bfloat16
NT = (((1,), (1,)), ((), ()))
TN = (((0,), (0,)), ((), ()))


def iota(shape, dim):
    return lax.broadcasted_iota(jnp.int32, shape, dim)


def mm(a, b):
    return jnp.dot(a, b, preferred_element_type=F32)


def silu(v):
    return v * jax.nn.sigmoid(v)


def layer(
    sizes,
    tok, w0, w1, w2, w3, w4, w5, state, mix_gain, decay_base, rate_base, head_gain, moe_gain, routing,
    gate_hbm, up_hbm, down_hbm, sgate_hbm, sup_hbm, sdown_hbm,
    out,
    wbuf, xs, xg, tg, gt, ut, dt, vs, vg, perm, seg, st, nh, prod,
    ps, pr, ms, mg, ao, ar, resid, ns, zg, sgv, suv, sdv, sh, shr,
    dmat, cmat, xsel, er, gs, gr, hs, hr, ob, cb, rb, zr,
    s_send, s_ring, s_xg, s_tg, s_gt, s_ut, s_dt, s_vg, s_pr, s_mg, s_ar, s_zg, s_shr, s_er, s_gr, s_hr, s_cb, s_zr,
    s_loc,
):
    nz, nx, nc, ny = sizes
    nxc = nx * nc
    rows, q = tok.shape
    zb = nz // ny
    heads = q // HEAD
    topk = routing.shape[0] // 2
    weights = (w0, w1, w2, w3, w4, w5)
    z, x, c, y = (lax.axis_index(a) for a in AXES)
    xc = x * nc + c
    sends = []

    def send(src, dst, recv_sem, where):
        copy = pltpu.make_async_remote_copy(
            src_ref=src, dst_ref=dst, send_sem=s_send.at[len(sends)], recv_sem=recv_sem,
            device_id=where, device_id_type=MESH_ID,
        )
        copy.start()
        sends.append(copy)

    def arrived(dst, recv_sem):
        pltpu.make_async_remote_copy(
            src_ref=dst, dst_ref=dst, send_sem=s_send.at[0], recv_sem=recv_sem,
            device_id=(z, x, c, y), device_id_type=MESH_ID,
        ).wait_recv()

    xc_off = [(dx, dc) for dx in range(nx) for dc in range(nc)]

    def xc_at(off):
        px, pc = lax.rem(x + off[0], nx), lax.rem(c + off[1], nc)
        return px, pc, px * nc + pc

    def y_at(dy):
        return lax.rem(y + dy, ny)

    def z_at(dz):
        return lax.rem(z + dz, nz)

    plane_off = [(o, dy) for o in xc_off for dy in range(ny)][1:]

    def at_lanes(i):
        return pl.ds(pl.multiple_of(i * LANES, LANES), LANES)

    local = []

    def load(src, dst):
        copy = pltpu.make_async_copy(src, dst, s_loc.at[len(local)])
        copy.start()
        local.append(copy)
        return copy

    own_rows = pl.ds(pl.multiple_of(y * q, q), q)
    load_gate = load(gate_hbm.at[own_rows, :], gt.at[y])
    load_up = load(up_hbm.at[own_rows, :], ut.at[y])
    load_down = load(down_hbm.at[:, own_rows], dt.at[y])
    load_state = load(state, st)
    load_sg = load(sgate_hbm, sgv)
    load_su = load(sup_hbm, suv)
    load_sd = load(sdown_hbm, sdv)

    tok32 = tok[...].astype(F32)
    rows_in = (tok32 * mix_gain[...]).astype(BF16)
    xs[...] = rows_in
    xg[xc] = rows_in
    tg[y] = tok[...]
    for m in range(6):
        wbuf[z // zb, m, lax.rem(z, zb)] = weights[m][...]

    barrier = pltpu.get_barrier_semaphore()
    for off, dy in plane_off:
        px, pc, _ = xc_at(off)
        pl.semaphore_signal(barrier, inc=1, device_id=(z, px, pc, y_at(dy)), device_id_type=MESH_ID)
    for dz in range(1, nz):
        pl.semaphore_signal(barrier, inc=1, device_id=(z_at(dz), x, c, y), device_id_type=MESH_ID)
    pl.semaphore_wait(barrier, len(plane_off) + nz - 1)

    half = nz // 2
    to_next, to_prev = (z_at(1), x, c, y), (z_at(nz - 1), x, c, y)
    for m in range(6):
        spot = wbuf.at[z // zb, m, lax.rem(z, zb)]
        send(weights[m], spot, s_ring.at[0, 0, m], to_next)
        send(weights[m], spot, s_ring.at[1, 0, m], to_prev)
    for off in xc_off[1:]:
        px, pc, _ = xc_at(off)
        send(xs, xg.at[xc], s_xg.at[xc], (z, px, pc, y))
    for dy in range(1, ny):
        send(tok, tg.at[y], s_tg.at[y], (z, x, c, y_at(dy)))
    for dy in range(1, ny):
        theirs = pl.ds(pl.multiple_of(y_at(dy) * q, q), q)
        send(gate_hbm.at[theirs, :], gt.at[y], s_gt.at[y], (z, x, c, y_at(dy)))
        send(up_hbm.at[theirs, :], ut.at[y], s_ut.at[y], (z, x, c, y_at(dy)))

    score = routing[topk : 2 * topk, :]
    share = score / jnp.sum(score, axis=0, keepdims=True) * ROUTED_SCALE
    experts = vs.shape[0]
    lane = iota((experts, LANES), 1)
    expert_id = iota((experts, LANES), 0).astype(F32)
    value = jnp.zeros((experts, LANES), F32)
    for k in range(topk):
        value += jnp.where(expert_id == routing[k : k + 1, :], share[k : k + 1, :], 0.0)
    same_block = (iota((LANES, LANES), 0) // rows == iota((LANES, LANES), 1) // rows) & (
        iota((LANES, LANES), 0) < iota((LANES, LANES), 1)
    )
    before = mm((value > 0.0).astype(BF16), same_block.astype(BF16))
    signed = jnp.where(before > 0.5, -value, value)
    vs[...] = jnp.where(lane // rows == lax.rem(z, LANES // rows), signed, 0.0)

    width = nxc * LANES
    strip = nxc * 16
    for i in range(nxc):
        r = iota((LANES, width), 0)
        goal = (r // 16) * strip + i * 16 + lax.rem(r, 16)
        perm[i * LANES : (i + 1) * LANES, :] = (iota((LANES, width), 1) == goal).astype(BF16)
    for j in range(HEAD // 2):
        r = iota((LANES, LANES), 0)
        goal = 2 * j + r // HEAD
        seg[j * LANES : (j + 1) * LANES, :] = (lax.rem(iota((LANES, LANES), 1), HEAD) == goal).astype(BF16)

    for step in range(1, half + 1):
        up_src, down_src = z_at(nz - step), z_at(step)
        for m in range(6):
            if step < half or m < 3:
                spot = wbuf.at[up_src // zb, m, lax.rem(up_src, zb)]
                arrived(spot, s_ring.at[0, step - 1, m])
                if step + 1 < half or (step + 1 == half and m < 3):
                    send(spot, spot, s_ring.at[0, step, m], to_next)
            if step < half or m >= 3:
                spot = wbuf.at[down_src // zb, m, lax.rem(down_src, zb)]
                arrived(spot, s_ring.at[1, step - 1, m])
                if step + 1 < half or (step + 1 == half and m >= 3):
                    send(spot, spot, s_ring.at[1, step, m], to_prev)
        if step == 1:
            for dz in range(1, nz):
                zt = z_at(dz)
                send(vs.at[pl.ds(pl.multiple_of(zt * nxc, nxc), nxc), :], vg.at[z], s_vg.at[z], (zt, x, c, y))
            vg[z] = vs[pl.ds(pl.multiple_of(z * nxc, nxc), nxc), :]

    for off in xc_off[1:]:
        _, _, pxc = xc_at(off)
        arrived(xg.at[pxc], s_xg.at[pxc])
    left = xg[...].reshape(nxc * rows, q)
    for yt in range(ny):
        for pair in range(3):
            w = wbuf[yt, 2 * pair : 2 * pair + 2].reshape(LANES, q)
            part = lax.dot_general(left, w, NT, preferred_element_type=F32)
            ps[yt, :, pair] = part.astype(BF16).reshape(nxc, rows, LANES)
    for off, dy in plane_off:
        px, pc, pxc = xc_at(off)
        py = y_at(dy)
        send(ps.at[py, pxc], pr.at[y, :, :, at_lanes(xc)], s_pr.at[xc * ny + y], (z, px, pc, py))
    for dy in range(1, ny):
        theirs = pl.ds(pl.multiple_of(y_at(dy) * q, q), q)
        send(down_hbm.at[:, theirs], dt.at[y], s_dt.at[y], (z, x, c, y_at(dy)))
    pr[y, :, :, at_lanes(xc)] = ps[y, xc]

    for dy in range(1, ny):
        arrived(tg.at[y_at(dy)], s_tg.at[y_at(dy)])
    tok_all = tg[...].astype(F32)
    square = jnp.sum(jnp.sum(tok_all * tok_all, axis=0), axis=1, keepdims=True)
    factor = lax.rsqrt(square / (ny * q) + RMS_EPS)

    for off, dy in plane_off:
        _, _, pxc = xc_at(off)
        arrived(pr.at[y_at(dy), :, :, at_lanes(pxc)], s_pr.at[pxc * ny + y_at(dy)])
    spread = mm(pr[...].reshape(ny * 3 * rows, width), perm[...]).reshape(ny, 3, rows, width)
    summed = jnp.sum(spread, axis=0)
    low = iota((rows, LANES), 1) < HEAD
    for m in range(5):
        flat = summed[m // 2, :, (m % 2) * q : (m % 2 + 1) * q] * factor
        if m == 3:
            flat = flat + decay_base[...]
        if m == 4:
            flat = flat + rate_base[...]
        for t in range(q // LANES):
            here = flat[:, t * LANES : (t + 1) * LANES]
            swapped = pltpu.roll(here, HEAD, 1)
            nh[m, pl.ds(2 * t, rows, stride=heads), :] = jnp.where(low, here, swapped)
            nh[m, pl.ds(2 * t + 1, rows, stride=heads), :] = jnp.where(low, swapped, here)

    def head_sum(v):
        return 0.5 * jnp.sum(v, axis=1, keepdims=True)

    receptance, key, val = nh[0], nh[1], nh[2]
    decay = jnp.exp(-jnp.exp(-jax.nn.softplus(-nh[3]) - 0.5))
    in_rate = jax.nn.sigmoid(nh[4])
    unit = key * lax.rsqrt(head_sum(key * key) + KEY_EPS)
    rated = in_rate * receptance
    mix_w = decay * receptance - head_sum(unit * rated) * unit
    fed = head_sum(key * rated)
    load_state.wait()
    for j in range(HEAD // 2):
        block = st[:, :, j * LANES : (j + 1) * LANES].astype(F32).reshape(rows * heads, LANES)
        prod[:, j * LANES : (j + 1) * LANES] = (block * mix_w).astype(BF16)
    readout = mm(prod[...], seg[...]) + fed * val
    centre = jnp.sum(readout, axis=1, keepdims=True) / LANES
    moved = readout - centre
    var = jnp.sum(moved * moved, axis=1, keepdims=True) / LANES
    nh[0] = moved * lax.rsqrt(var + GN_EPS)
    for t in range(q // LANES):
        even = nh[0, pl.ds(2 * t, rows, stride=heads), :]
        odd = nh[0, pl.ds(2 * t + 1, rows, stride=heads), :]
        cols = slice(t * LANES, (t + 1) * LANES)
        ms[:, cols] = (jnp.where(low, even, odd) * head_gain[:, cols]).astype(BF16)

    for off in xc_off[1:]:
        px, pc, _ = xc_at(off)
        send(ms, mg.at[xc], s_mg.at[xc], (z, px, pc, y))
    mg[xc] = ms[...]
    for off in xc_off[1:]:
        _, _, pxc = xc_at(off)
        arrived(mg.at[pxc], s_mg.at[pxc])
    left = mg[...].reshape(nxc * rows, q)
    per = 8 // zb
    for zh in range(nz // 8):
        w = wbuf[per * zh : per * (zh + 1), 5].reshape(LANES, q)
        part = lax.dot_general(left, w, NT, preferred_element_type=F32)
        ao[:, zh] = part.astype(BF16).reshape(nxc, rows, LANES)
    for off, dy in plane_off:
        px, pc, pxc = xc_at(off)
        send(ao.at[pxc], ar.at[y, :, :, at_lanes(xc)], s_ar.at[xc * ny + y], (z, px, pc, y_at(dy)))
    ar[y, :, :, at_lanes(xc)] = ao[xc]
    for off, dy in plane_off:
        _, _, pxc = xc_at(off)
        arrived(ar.at[y_at(dy), :, :, at_lanes(pxc)], s_ar.at[pxc * ny + y_at(dy)])
    spread = mm(ar[...].reshape(ny * (nz // 8) * rows, width), perm[...]).reshape(ny, nz // 8, rows, width)
    summed = jnp.sum(spread, axis=0)
    per = width // q
    square = jnp.zeros((rows, 1), F32)
    for i in range(ny):
        attended = summed[i // per, :, (i % per) * q : (i % per + 1) * q]
        resid[i] = (tg[i].astype(F32) + attended).astype(BF16)
        r32 = resid[i].astype(F32)
        square += jnp.sum(r32 * r32, axis=1, keepdims=True)
    factor = lax.rsqrt(square / (ny * q) + RMS_EPS)
    for i in range(ny):
        ns[i] = (resid[i].astype(F32) * factor * moe_gain[:, i * q : (i + 1) * q]).astype(BF16)

    for dz in range(1, nz):
        send(ns.at[y], zg.at[z], s_zg.at[z], (z_at(dz), x, c, y))
    zg[z] = ns[y]

    load_sg.wait()
    load_su.wait()
    load_sd.wait()
    hid_g = jnp.zeros((rows, LANES), F32)
    hid_u = jnp.zeros((rows, LANES), F32)
    for i in range(ny):
        hid_g += mm(ns[i], sgv[i * q : (i + 1) * q, :])
        hid_u += mm(ns[i], suv[i * q : (i + 1) * q, :])
    hid = (silu(hid_g) * hid_u).astype(BF16)
    for i in range(ny):
        sh[i] = mm(hid, sdv[:, i * q : (i + 1) * q]).astype(BF16)
    for dy in range(1, ny):
        send(sh.at[y_at(dy)], shr.at[y], s_shr.at[y], (z, x, c, y_at(dy)))
    shr[y] = sh[y]

    for dz in range(1, nz):
        arrived(vg.at[z_at(dz)], s_vg.at[z_at(dz)])
    per = LANES // rows
    table = jnp.concatenate([jnp.sum(vg[h * per : (h + 1) * per], axis=0) for h in range(nz // per)], axis=1)
    shape = (2 * nz, nz * rows)
    mine = iota(shape, 0) // 2 == iota(shape, 1) // rows
    sign = jnp.where(lax.rem(iota(shape, 0), 2) == 0, 1.0, -1.0)
    for i in range(nxc):
        weight = jnp.where(mine, table[i : i + 1, :] * sign, 0.0)
        spot = slice(i * 2 * nz, (i + 1) * 2 * nz)
        dmat[spot, :] = (weight > 0.0).astype(BF16)
        cmat[spot, :] = jnp.maximum(weight, 0.0).astype(BF16)

    for dz in range(1, nz):
        arrived(zg.at[z_at(dz)], s_zg.at[z_at(dz)])
    picked = mm(dmat[...], zg[...].reshape(nz * rows, q)).astype(BF16)
    xsel[...] = picked.reshape(nxc, 2 * nz, q)
    for off in xc_off[1:]:
        px, pc, pxc = xc_at(off)
        send(xsel.at[pxc], er.at[xc], s_er.at[xc], (z, px, pc, y))
    er[xc] = xsel[xc]

    load_gate.wait()
    load_up.wait()
    load_down.wait()
    for dy in range(1, ny):
        arrived(gt.at[y_at(dy)], s_gt.at[y_at(dy)])
        arrived(ut.at[y_at(dy)], s_ut.at[y_at(dy)])
        arrived(dt.at[y_at(dy)], s_dt.at[y_at(dy)])
    for off in xc_off[1:]:
        _, _, pxc = xc_at(off)
        arrived(er.at[pxc], s_er.at[pxc])
    chosen = er[...].reshape(nxc * 2 * nz, q)
    for i in range(ny):
        gs[i, :, 0:LANES] = mm(chosen, gt[i]).astype(BF16)
        gs[i, :, LANES : 2 * LANES] = mm(chosen, ut[i]).astype(BF16)
    for dy in range(1, ny):
        send(gs.at[y_at(dy)], gr.at[y], s_gr.at[y], (z, x, c, y_at(dy)))
    gr[y] = gs[y]
    for dy in range(1, ny):
        arrived(gr.at[y_at(dy)], s_gr.at[y_at(dy)])
    pre = jnp.sum(gr[...].astype(F32), axis=0)
    hs[...] = (silu(pre[:, 0:LANES]) * pre[:, LANES : 2 * LANES]).astype(BF16)
    for dy in range(1, ny):
        send(hs, hr.at[y], s_hr.at[y], (z, x, c, y_at(dy)))
    hr[y] = hs[...]
    for dy in range(1, ny):
        arrived(hr.at[y_at(dy)], s_hr.at[y_at(dy)])
    total = mm(hr[0], dt[0])
    for i in range(1, ny):
        total += mm(hr[i], dt[i])
    ob[...] = total.astype(BF16).reshape(nxc, 2 * nz, q)
    for off in xc_off[1:]:
        px, pc, pxc = xc_at(off)
        send(ob.at[pxc], cb.at[xc], s_cb.at[xc], (z, px, pc, y))
    cb[xc] = ob[xc]
    for off in xc_off[1:]:
        _, _, pxc = xc_at(off)
        arrived(cb.at[pxc], s_cb.at[pxc])

    routed = lax.dot_general(cmat[...], cb[...].reshape(nxc * 2 * nz, q), TN, preferred_element_type=F32)
    rb[...] = routed.astype(BF16).reshape(nz, rows, q)
    for dz in range(1, nz):
        send(rb.at[z_at(dz)], zr.at[z], s_zr.at[z], (z_at(dz), x, c, y))
    zr[z] = rb[z]
    for dy in range(1, ny):
        arrived(shr.at[y_at(dy)], s_shr.at[y_at(dy)])
    for dz in range(1, nz):
        arrived(zr.at[z_at(dz)], s_zr.at[z_at(dz)])
    final = resid[y].astype(F32) + jnp.sum(zr[...].astype(F32), axis=0) + jnp.sum(shr[...].astype(F32), axis=0)
    out[...] = final.astype(BF16)
    for copy in sends:
        copy.wait_send()


def body(
    tokens, state, mix_gain, w_recept, w_key, w_value, w_decay, w_rate, decay_base, rate_base, head_gain, w_out,
    moe_gain, routes, route_weight, expert_gate, expert_up, expert_down, shared_gate, shared_up, shared_down,
):
    sizes = tuple(lax.axis_size(a) for a in AXES)
    nz, nx, nc, ny = sizes
    nxc = nx * nc
    rows, q = tokens.shape
    heads = q // HEAD
    routing = jnp.concatenate([routes.T.astype(F32), route_weight.T], axis=0)
    routing = jnp.tile(routing, (1, LANES // rows))
    turned = [w.T for w in (w_recept, w_key, w_value, w_decay, w_rate, w_out)]
    line = [v[None, :] for v in (mix_gain, decay_base, rate_base, head_gain, moe_gain)]
    vmem = pl.BlockSpec(memory_space=pltpu.VMEM)
    hbm = pl.BlockSpec(memory_space=pl.ANY)
    slots = 2 * nz
    count = nxc * slots
    width = nxc * LANES

    def vb(*shape):
        return pltpu.VMEM(shape, BF16)

    def vf(*shape):
        return pltpu.VMEM(shape, F32)

    dma = pltpu.SemaphoreType.DMA
    plane = nxc * ny - 1
    half = nz // 2
    ring = 2 * (6 + 6 * (half - 2) + 3)
    n_sends = ring + 5 * (nxc - 1) - (nxc - 1) + (ny - 1) * 7 + 3 * (nz - 1) + 2 * plane
    scratch = [
        vb(ny, 6, nz // ny, 16, q), vb(rows, q), vb(nxc, rows, q), vb(ny, rows, q),
        vb(ny, q, LANES), vb(ny, q, LANES), vb(ny, LANES, q), vf(nz * nxc, LANES), vf(nz, nxc, LANES),
        vb(width, width), vb(HEAD * HEAD, LANES), vb(rows, heads, HEAD * HEAD), vf(5, rows * heads, LANES),
        vb(rows * heads, HEAD * HEAD),
        vb(ny, nxc, 3, rows, LANES), vb(ny, 3, rows, width), vb(rows, q), vb(nxc, rows, q),
        vb(nxc, nz // 8, rows, LANES), vb(ny, nz // 8, rows, width), vb(ny, rows, q), vb(ny, rows, q),
        vb(nz, rows, q), vb(ny * q, LANES), vb(ny * q, LANES), vb(LANES, ny * q), vb(ny, rows, q), vb(ny, rows, q),
        vb(count, nz * rows), vb(count, nz * rows), vb(nxc, slots, q), vb(nxc, slots, q),
        vb(ny, count, 2 * LANES), vb(ny, count, 2 * LANES), vb(count, LANES), vb(ny, count, LANES),
        vb(nxc, slots, q), vb(nxc, slots, q), vb(nz, rows, q), vb(nz, rows, q),
        dma((n_sends,)), dma((2, half, 6)), dma((nxc,)), dma((ny,)), dma((ny,)), dma((ny,)), dma((ny,)), dma((nz,)),
        dma((nxc * ny,)), dma((nxc,)), dma((nxc * ny,)), dma((nz,)), dma((ny,)), dma((nxc,)), dma((ny,)), dma((ny,)),
        dma((nxc,)), dma((nz,)), dma((7,)),
    ]
    return pl.pallas_call(
        functools.partial(layer, sizes),
        out_shape=jax.ShapeDtypeStruct((rows, q), BF16),
        in_specs=[vmem] * 7 + [hbm] + [vmem] * 6 + [hbm] * 6,
        out_specs=vmem,
        scratch_shapes=scratch,
        compiler_params=pltpu.CompilerParams(
            collective_id=0, has_side_effects=True, vmem_limit_bytes=48 * 1024 * 1024
        ),
        name="layer",
    )(
        tokens, *turned, state, *line, routing,
        expert_gate[0], expert_up[0], expert_down[0], shared_gate, shared_up, shared_down,
    )


def solution(mesh):
    shape = SHAPE if SHAPE else (16, 4, 2, mesh.shape["tp"])
    torus = Mesh(mesh.devices.reshape(shape), AXES)
    placed = (
        P(EP, "tp"), P(EP, "tp", None), P("tp"),
        P("tp", EP), P("tp", EP), P("tp", EP), P("tp", EP), P("tp", EP),
        P("tp"), P("tp"), P("tp"), P("tp", EP), P(), P(EP, None), P(EP, None),
        P(EP, None, "tp"), P(EP, None, "tp"), P(EP, "tp", None), P(None, "tp"), P(None, "tp"), P("tp", None),
    )
    return jax.shard_map(body, mesh=torus, in_specs=placed, out_specs=P(EP, "tp"), check_vma=False)


SHAPE = None
```

```python
import functools

import jax
import jax.numpy as jnp
from jax import lax
from jax.experimental import pallas as pl
from jax.experimental.pallas import tpu as pltpu
from jax.sharding import Mesh
from jax.sharding import PartitionSpec as P

HEAD = 64
LANES = 128
RMS_EPS = 1e-06
GN_EPS = 0.00064
KEY_EPS = 1e-06
ROUTED_SCALE = 2.5
AXES = ("ep_0", "ep_1", "ep_2", "tp")
EP = AXES[:3]
MESH_ID = pl.DeviceIdType.MESH
F32 = jnp.float32
BF16 = jnp.bfloat16
NT = (((1,), (1,)), ((), ()))
TN = (((0,), (0,)), ((), ()))


def iota(shape, dim):
    return lax.broadcasted_iota(jnp.int32, shape, dim)


def mm(a, b):
    return jnp.dot(a, b, preferred_element_type=F32)


def silu(v):
    return v * jax.nn.sigmoid(v)


def layer(
    sizes,
    tok_hbm, w0, w1, w2, w3, w4, w5, state, mix_hbm, dbase_hbm, rbase_hbm, hgain_hbm, mgain_hbm, routes_hbm, score_hbm,
    gate_hbm, up_hbm, down_hbm, sgate_hbm, sup_hbm, sdown_hbm,
    out,
    tok, mix_gain, decay_base, rate_base, head_gain, moe_gain, routes, score,
    wbuf, wo, xs, xg, tg, gt, ut, dt, vs, vg, perm, seg, st, nh, prod,
    ps, pr, ms, po, ar, resid, ns, zg, sgv, suv, sdv, sh, shr,
    dmat, cmat, xsel, er, gs, gr, hs, hr, ob, cb, rb, zr, zp, z8, za,
    s_send, s_ring, s_wx, s_wc, s_xg, s_tg, s_gt, s_ut, s_dt, s_vg, s_pr, s_ar, s_zg, s_shr, s_er, s_gr, s_hr, s_cb,
    s_zr, s_zp, s_z8, s_loc,
):
    nz, nx, nc, ny = sizes
    nxc = nx * nc
    rows, q = tok.shape
    zb = nz // ny
    heads = q // HEAD
    topk = routes.shape[0]
    weights = (w0, w1, w2, w3, w4, w5)
    half, quart = nz // 2, nz // 4
    order = [0, *[i for k in range(1, half) for i in (k, -k)], half]
    place = {r % nz: p for p, r in enumerate(order)}
    z, x, c, y = (lax.axis_index(a) for a in AXES)
    xc = x * nc + c
    sends = []

    def send(src, dst, recv_sem, where):
        copy = pltpu.make_async_remote_copy(
            src_ref=src, dst_ref=dst, send_sem=s_send.at[len(sends)], recv_sem=recv_sem,
            device_id=where, device_id_type=MESH_ID,
        )
        copy.start()
        sends.append(copy)

    def arrived(dst, recv_sem):
        pltpu.make_async_remote_copy(
            src_ref=dst, dst_ref=dst, send_sem=s_send.at[0], recv_sem=recv_sem,
            device_id=(z, x, c, y), device_id_type=MESH_ID,
        ).wait_recv()

    xc_off = [(dx, dc) for dx in range(nx) for dc in range(nc)]

    def xc_at(off):
        px, pc = lax.rem(x + off[0], nx), lax.rem(c + off[1], nc)
        return px, pc, px * nc + pc

    def y_at(dy):
        return lax.rem(y + dy, ny)

    def z_at(dz):
        return lax.rem(z + dz, nz)

    plane_off = [(o, dy) for o in xc_off for dy in range(ny)][1:]

    def at_lanes(i):
        return pl.ds(pl.multiple_of(i * LANES, LANES), LANES)

    local = []

    def load(src, dst):
        copy = pltpu.make_async_copy(src, dst, s_loc.at[len(local)])
        copy.start()
        local.append(copy)
        return copy

    def block(m, source):
        return wo.at[xc, source] if m == 5 else wbuf.at[source // zb, m, lax.rem(source, zb)]

    first = [load(tok_hbm, tok), load(mix_hbm, mix_gain), load(routes_hbm, routes), load(score_hbm, score)]
    own_w = [load(weights[m], block(m, z)) for m in range(6)]
    bases = [load(dbase_hbm, decay_base), load(rbase_hbm, rate_base), load(hgain_hbm, head_gain)]
    bases.append(load(mgain_hbm, moe_gain))
    load_state = load(state, st)
    own_rows = pl.ds(pl.multiple_of(y * q, q), q)
    load_gate = load(gate_hbm.at[own_rows, :], gt.at[y])
    load_up = load(up_hbm.at[own_rows, :], ut.at[y])
    load_down = load(down_hbm.at[:, own_rows], dt.at[y])
    load_sg = load(sgate_hbm, sgv)
    load_su = load(sup_hbm, suv)
    load_sd = load(sdown_hbm, sdv)

    width = nxc * LANES
    strip = nxc * 16
    for i in range(nxc):
        r = iota((LANES, width), 0)
        goal = (r // 16) * strip + i * 16 + lax.rem(r, 16)
        perm[i * LANES : (i + 1) * LANES, :] = (iota((LANES, width), 1) == goal).astype(BF16)
    for j in range(HEAD // 2):
        r = iota((LANES, LANES), 0)
        goal = 2 * j + r // HEAD
        seg[j * LANES : (j + 1) * LANES, :] = (lax.rem(iota((LANES, LANES), 1), HEAD) == goal).astype(BF16)

    for copy in first:
        copy.wait()
    rows_in = (tok[...].astype(F32) * mix_gain[...]).astype(BF16)
    xs[...] = rows_in
    xg[xc] = rows_in
    tg[y] = tok[...]

    spreader = (lax.rem(iota((rows, LANES), 1), rows) == iota((rows, LANES), 0)).astype(F32)
    exact = functools.partial(jnp.dot, preferred_element_type=F32, precision=lax.Precision.HIGHEST)
    share = score[...] / jnp.sum(score[...], axis=0, keepdims=True) * ROUTED_SCALE
    route_lanes = exact(routes[...].astype(F32), spreader)
    share_lanes = exact(share, spreader)
    experts = vs.shape[0]
    expert_id = iota((experts, LANES), 0).astype(F32)
    value = jnp.zeros((experts, LANES), F32)
    for k in range(topk):
        value += jnp.where(jnp.abs(expert_id - route_lanes[k : k + 1, :]) < 0.5, share_lanes[k : k + 1, :], 0.0)
    same_block = (iota((LANES, LANES), 0) // rows == iota((LANES, LANES), 1) // rows) & (
        iota((LANES, LANES), 0) < iota((LANES, LANES), 1)
    )
    before = mm((value > 0.0).astype(BF16), same_block.astype(BF16))
    vs[...] = jnp.where(before > 0.5, -value, value)
    for copy in own_w:
        copy.wait()

    barrier = pltpu.get_barrier_semaphore()
    for off, dy in plane_off:
        px, pc, _ = xc_at(off)
        pl.semaphore_signal(barrier, inc=1, device_id=(z, px, pc, y_at(dy)), device_id_type=MESH_ID)
    for dz in range(1, nz):
        pl.semaphore_signal(barrier, inc=1, device_id=(z_at(dz), x, c, y), device_id_type=MESH_ID)
    pl.semaphore_wait(barrier, len(plane_off) + nz - 1)

    to_next, to_prev = (z_at(1), x, c, y), (z_at(nz - 1), x, c, y)
    ring = (5, 0, 1, 2, 3, 4)
    split = ring[:3]
    for m in ring:
        spot = block(m, z)
        send(spot, spot, s_ring.at[0, 0, m], to_next)
        send(spot, spot, s_ring.at[1, 0, m], to_prev)

    def pass_along_x(source):
        for dx in range(1, nx):
            px = lax.rem(x + dx, nx)
            send(wo.at[xc, source], wo.at[xc, source], s_wx.at[x, source], (z, px, c, y))

    pass_along_x(z)
    for off in xc_off[1:]:
        px, pc, _ = xc_at(off)
        send(xs, xg.at[xc], s_xg.at[xc], (z, px, pc, y))
    for dy in range(1, ny):
        send(tok, tg.at[y], s_tg.at[y], (z, x, c, y_at(dy)))
    for dy in range(1, ny):
        theirs = pl.ds(pl.multiple_of(y_at(dy) * q, q), q)
        send(gate_hbm.at[theirs, :], gt.at[y], s_gt.at[y], (z, x, c, y_at(dy)))
        send(up_hbm.at[theirs, :], ut.at[y], s_ut.at[y], (z, x, c, y_at(dy)))
    for dy in range(1, ny):
        theirs = pl.ds(pl.multiple_of(y_at(dy) * q, q), q)
        send(down_hbm.at[:, theirs], dt.at[y], s_dt.at[y], (z, x, c, y_at(dy)))

    for step in range(1, half + 1):
        up_src, down_src = z_at(nz - step), z_at(step)
        for m in ring:
            if step < half or m in split:
                spot = block(m, up_src)
                arrived(spot, s_ring.at[0, step - 1, m])
                if step + 1 < half or (step + 1 == half and m in split):
                    send(spot, spot, s_ring.at[0, step, m], to_next)
                if m == 5:
                    pass_along_x(up_src)
            if step < half or m not in split:
                spot = block(m, down_src)
                arrived(spot, s_ring.at[1, step - 1, m])
                if step + 1 < half or (step + 1 == half and m not in split):
                    send(spot, spot, s_ring.at[1, step, m], to_prev)
                if m == 5:
                    pass_along_x(down_src)

    for off in xc_off[1:]:
        _, _, pxc = xc_at(off)
        arrived(xg.at[pxc], s_xg.at[pxc])
    left = xg[...].reshape(nxc * rows, q)
    for yt in range(ny):
        for pair in range(3):
            first_m = min(2 * pair, 3)
            w = wbuf[yt, first_m : first_m + 2].reshape(LANES, q)
            part = lax.dot_general(left, w, NT, preferred_element_type=F32)
            ps[yt, :, pair] = part.astype(BF16).reshape(nxc, rows, LANES)
    for off, dy in plane_off:
        px, pc, pxc = xc_at(off)
        py = y_at(dy)
        send(ps.at[py, pxc], pr.at[y, :, :, at_lanes(xc)], s_pr.at[xc * ny + y], (z, px, pc, py))
    def rows_of(zt):
        return vs.at[pl.ds(pl.multiple_of(zt * nxc, nxc), nxc), :]

    for r in range(1, nz):
        send(rows_of(z_at(r)), vg.at[place[-r % nz]], s_vg.at[place[-r % nz]], (z_at(r), x, c, y))
    vg[0] = vs[pl.ds(pl.multiple_of(z * nxc, nxc), nxc), :]
    pr[y, :, :, at_lanes(xc)] = ps[y, xc]

    for dy in range(1, ny):
        arrived(tg.at[y_at(dy)], s_tg.at[y_at(dy)])
    tok_all = tg[...].astype(F32)
    square = jnp.sum(jnp.sum(tok_all * tok_all, axis=0), axis=1, keepdims=True)
    factor = lax.rsqrt(square / (ny * q) + RMS_EPS)

    for off, dy in plane_off:
        _, _, pxc = xc_at(off)
        arrived(pr.at[y_at(dy), :, :, at_lanes(pxc)], s_pr.at[pxc * ny + y_at(dy)])
    for dx in range(1, nx):
        px = lax.rem(x + dx, nx)
        for source in range(nz):
            arrived(wo.at[px * nc + c, source], s_wx.at[px, source])
    for px in range(nx):
        for dc in range(1, nc):
            send(wo.at[px * nc + c], wo.at[px * nc + c], s_wc.at[px], (z, x, lax.rem(c + dc, nc), y))
    for copy in bases:
        copy.wait()
    spread = mm(pr[...].reshape(ny * 3 * rows, width), perm[...]).reshape(ny, 3, rows, width)
    summed = jnp.sum(spread, axis=0)
    low = iota((rows, LANES), 1) < HEAD
    for m in range(5):
        group, side = (2, 1) if m == 4 else (m // 2, m % 2)
        flat = summed[group, :, side * q : (side + 1) * q] * factor
        if m == 3:
            flat = flat + decay_base[...]
        if m == 4:
            flat = flat + rate_base[...]
        for t in range(q // LANES):
            here = flat[:, t * LANES : (t + 1) * LANES]
            swapped = pltpu.roll(here, HEAD, 1)
            nh[m, pl.ds(2 * t, rows, stride=heads), :] = jnp.where(low, here, swapped)
            nh[m, pl.ds(2 * t + 1, rows, stride=heads), :] = jnp.where(low, swapped, here)

    def head_sum(v):
        return 0.5 * jnp.sum(v, axis=1, keepdims=True)

    receptance, key, val = nh[0], nh[1], nh[2]
    decay = jnp.exp(-jnp.exp(-jax.nn.softplus(-nh[3]) - 0.5))
    in_rate = jax.nn.sigmoid(nh[4])
    unit = key * lax.rsqrt(head_sum(key * key) + KEY_EPS)
    rated = in_rate * receptance
    mix_w = decay * receptance - head_sum(unit * rated) * unit
    fed = head_sum(key * rated)
    load_state.wait()
    for j in range(HEAD // 2):
        block = st[:, :, j * LANES : (j + 1) * LANES].astype(F32).reshape(rows * heads, LANES)
        prod[:, j * LANES : (j + 1) * LANES] = (block * mix_w).astype(BF16)
    readout = mm(prod[...], seg[...]) + fed * val
    centre = jnp.sum(readout, axis=1, keepdims=True) / LANES
    moved = readout - centre
    var = jnp.sum(moved * moved, axis=1, keepdims=True) / LANES
    nh[0] = moved * lax.rsqrt(var + GN_EPS)
    for t in range(q // LANES):
        even = nh[0, pl.ds(2 * t, rows, stride=heads), :]
        odd = nh[0, pl.ds(2 * t + 1, rows, stride=heads), :]
        cols = slice(t * LANES, (t + 1) * LANES)
        ms[:, cols] = (jnp.where(low, even, odd) * head_gain[:, cols]).astype(BF16)

    for px in range(nx):
        for dc in range(1, nc):
            arrived(wo.at[px * nc + lax.rem(c + dc, nc)], s_wc.at[px])
    mixed = ms[...]
    for i in range(nxc):
        for zh in range(nz // 8):
            w = wo[i, 8 * zh : 8 * (zh + 1)].reshape(LANES, q)
            part = lax.dot_general(mixed, w, NT, preferred_element_type=F32)
            po[zh, :, i * LANES : (i + 1) * LANES] = part.astype(BF16)
    for dy in range(1, ny):
        send(po, ar.at[y], s_ar.at[y], (z, x, c, y_at(dy)))
    ar[y] = po[...]
    for dy in range(1, ny):
        arrived(ar.at[y_at(dy)], s_ar.at[y_at(dy)])
    spread = mm(ar[...].reshape(ny * (nz // 8) * rows, width), perm[...]).reshape(ny, nz // 8, rows, width)
    summed = jnp.sum(spread, axis=0)
    per = width // q
    square = jnp.zeros((rows, 1), F32)
    for i in range(ny):
        attended = summed[i // per, :, (i % per) * q : (i % per + 1) * q]
        resid[i] = (tg[i].astype(F32) + attended).astype(BF16)
        r32 = resid[i].astype(F32)
        square += jnp.sum(r32 * r32, axis=1, keepdims=True)
    factor = lax.rsqrt(square / (ny * q) + RMS_EPS)
    for i in range(ny):
        ns[i] = (resid[i].astype(F32) * factor * moe_gain[:, i * q : (i + 1) * q]).astype(BF16)

    for k in range(quart, 0, -1):
        for r in (k, -k):
            spot = place[-r % nz]
            send(ns.at[y], zg.at[spot], s_zg.at[spot], (z_at(r % nz), x, c, y))
    zg[0] = ns[y]

    load_sg.wait()
    load_su.wait()
    load_sd.wait()
    hid_g = jnp.zeros((rows, LANES), F32)
    hid_u = jnp.zeros((rows, LANES), F32)
    for i in range(ny):
        hid_g += mm(ns[i], sgv[i * q : (i + 1) * q, :])
        hid_u += mm(ns[i], suv[i * q : (i + 1) * q, :])
    hid = (silu(hid_g) * hid_u).astype(BF16)
    for i in range(ny):
        sh[i] = mm(hid, sdv[:, i * q : (i + 1) * q]).astype(BF16)
    for dy in range(1, ny):
        send(sh.at[y_at(dy)], shr.at[y], s_shr.at[y], (z, x, c, y_at(dy)))
    shr[y] = sh[y]

    for r in range(1, nz):
        arrived(vg.at[place[r]], s_vg.at[place[r]])
    lane_block = iota((nxc, LANES), 1) // rows
    shape = (2 * half, half * rows)
    mine = iota(shape, 0) // 2 == iota(shape, 1) // rows
    sign = jnp.where(lax.rem(iota(shape, 0), 2) == 0, 1.0, -1.0)
    for ch in range(2):
        table = jnp.zeros((nxc, LANES), F32)
        for p in range(half):
            table += jnp.where(lane_block == p, vg[ch * half + p], 0.0)
        for i in range(nxc):
            weight = jnp.where(mine, table[i : i + 1, 0 : half * rows] * sign, 0.0)
            spot = slice(i * 2 * half, (i + 1) * 2 * half)
            dmat[ch, spot, :] = (weight > 0.0).astype(BF16)
            cmat[ch, spot, :] = jnp.maximum(weight, 0.0).astype(BF16)

    def wait_zg(p):
        arrived(zg.at[p], s_zg.at[p])

    back, ahead = place[-quart % nz], place[quart]
    wait_zg(back)
    wait_zg(ahead)
    far = back + c * (ahead - back)
    spot = place[half]
    send(zg.at[far], zg.at[spot], s_zg.at[spot], (z_at(quart + c * (half if nc > 1 else 0)), x, c, y))
    for k in range(quart - 1, 0, -1):
        spot = place[-(quart + k) % nz]
        send(zg.at[back], zg.at[spot], s_zg.at[spot], (z_at(k), x, c, y))
        spot = place[quart + k]
        send(zg.at[ahead], zg.at[spot], s_zg.at[spot], (z_at(nz - k), x, c, y))

    def pick(ch):
        for p in range(ch * half, (ch + 1) * half):
            if p not in (0, back, ahead):
                wait_zg(p)
        chosen = mm(dmat[ch], zg[ch * half : (ch + 1) * half].reshape(half * rows, q)).astype(BF16)
        xsel[ch] = chosen.reshape(nxc, 2 * half, q)
        for off in xc_off[1:]:
            px, pc, pxc = xc_at(off)
            send(xsel.at[ch, pxc], er.at[ch, xc], s_er.at[ch, xc], (z, px, pc, y))
        er[ch, xc] = xsel[ch, xc]

    def gate_up(ch):
        for off in xc_off[1:]:
            _, _, pxc = xc_at(off)
            arrived(er.at[ch, pxc], s_er.at[ch, pxc])
        chosen = er[ch].reshape(nxc * 2 * half, q)
        for i in range(ny):
            gs[ch, i, :, 0:LANES] = mm(chosen, gt[i]).astype(BF16)
            gs[ch, i, :, LANES : 2 * LANES] = mm(chosen, ut[i]).astype(BF16)
        for dy in range(1, ny):
            send(gs.at[ch, y_at(dy)], gr.at[ch, y], s_gr.at[ch, y], (z, x, c, y_at(dy)))
        gr[ch, y] = gs[ch, y]

    def hidden(ch):
        for dy in range(1, ny):
            arrived(gr.at[ch, y_at(dy)], s_gr.at[ch, y_at(dy)])
        pre = jnp.sum(gr[ch].astype(F32), axis=0)
        hs[ch] = (silu(pre[:, 0:LANES]) * pre[:, LANES : 2 * LANES]).astype(BF16)
        for dy in range(1, ny):
            send(hs.at[ch], hr.at[ch, y], s_hr.at[ch, y], (z, x, c, y_at(dy)))
        hr[ch, y] = hs[ch]

    def down(ch):
        for dy in range(1, ny):
            arrived(hr.at[ch, y_at(dy)], s_hr.at[ch, y_at(dy)])
        total = mm(hr[ch, 0], dt[0])
        for i in range(1, ny):
            total += mm(hr[ch, i], dt[i])
        ob[ch] = total.astype(BF16).reshape(nxc, 2 * half, q)
        for off in xc_off[1:]:
            px, pc, pxc = xc_at(off)
            send(ob.at[ch, pxc], cb.at[ch, xc], s_cb.at[ch, xc], (z, px, pc, y))
        cb[ch, xc] = ob[ch, xc]

    def combine(ch):
        for off in xc_off[1:]:
            _, _, pxc = xc_at(off)
            arrived(cb.at[ch, pxc], s_cb.at[ch, pxc])
        back_rows = cb[ch].reshape(nxc * 2 * half, q)
        routed = lax.dot_general(cmat[ch], back_rows, TN, preferred_element_type=F32)
        rb[ch * half : (ch + 1) * half] = routed.astype(BF16).reshape(half, rows, q)
        for p in range(half * (ch + 1) - 1, half * ch - 1, -1):
            r = order[p]
            if 0 < abs(r) < quart:
                spot = place[-r % nz]
                send(rb.at[p], zr.at[spot], s_zr.at[spot], (z_at(r % nz), x, c, y))
            elif quart < abs(r) < half:
                way, hop = (0, r - quart) if r > 0 else (1, r + quart)
                send(rb.at[p], zp.at[way, abs(hop) - 1], s_zp.at[way, abs(hop) - 1], (z_at(hop % nz), x, c, y))
            elif r == half:
                send(rb.at[p], z8, s_z8, (z_at(quart + c * (half if nc > 1 else 0)), x, c, y))

    pick(0)
    load_gate.wait()
    load_up.wait()
    load_down.wait()
    for dy in range(1, ny):
        arrived(gt.at[y_at(dy)], s_gt.at[y_at(dy)])
        arrived(ut.at[y_at(dy)], s_ut.at[y_at(dy)])
        arrived(dt.at[y_at(dy)], s_dt.at[y_at(dy)])
    gate_up(0)
    pick(1)
    hidden(0)
    gate_up(1)
    down(0)
    hidden(1)
    combine(0)
    down(1)
    combine(1)

    for way in range(2):
        for k in range(quart - 1):
            arrived(zp.at[way, k], s_zp.at[way, k])
    arrived(z8, s_z8)
    for way, r in ((0, quart), (1, -quart)):
        mine_too = (1 - c).astype(F32) if way == 0 else c.astype(F32)
        joined = rb[place[r % nz]].astype(F32) + z8[...].astype(F32) * mine_too
        for k in range(quart - 1):
            joined += zp[way, k].astype(F32)
        za[way] = joined.astype(BF16)
        spot = place[-r % nz]
        send(za.at[way], zr.at[spot], s_zr.at[spot], (z_at(r % nz), x, c, y))
    final = resid[y].astype(F32) + rb[0].astype(F32)
    for dy in range(1, ny):
        arrived(shr.at[y_at(dy)], s_shr.at[y_at(dy)])
    final += jnp.sum(shr[...].astype(F32), axis=0)
    for k in range(1, quart + 1):
        for r in (k, -k):
            spot = place[r % nz]
            arrived(zr.at[spot], s_zr.at[spot])
            final += zr[spot].astype(F32)
    out[...] = final.astype(BF16)
    for copy in sends:
        copy.wait_send()


def body(
    tokens, state, mix_gain, w_recept, w_key, w_value, w_decay, w_rate, decay_base, rate_base, head_gain, w_out,
    moe_gain, routes, route_weight, expert_gate, expert_up, expert_down, shared_gate, shared_up, shared_down,
):
    sizes = tuple(lax.axis_size(a) for a in AXES)
    nz, nx, nc, ny = sizes
    nxc = nx * nc
    rows, q = tokens.shape
    heads = q // HEAD
    topk = routes.shape[1]
    turned = [w.T for w in (w_recept, w_key, w_value, w_decay, w_rate, w_out)]
    line = [v[None, :] for v in (mix_gain, decay_base, rate_base, head_gain, moe_gain)]
    vmem = pl.BlockSpec(memory_space=pltpu.VMEM)
    hbm = pl.BlockSpec(memory_space=pl.ANY)
    half = nz // 2
    slots = 2 * half
    count = nxc * slots
    width = nxc * LANES

    def vb(*shape):
        return pltpu.VMEM(shape, BF16)

    def vf(*shape):
        return pltpu.VMEM(shape, F32)

    dma = pltpu.SemaphoreType.DMA
    scratch = [
        vb(rows, q), vf(1, q), vf(1, q), vf(1, q), vf(1, q), vf(1, ny * q),
        pltpu.VMEM((topk, rows), jnp.int32), vf(topk, rows),
        vb(ny, 5, nz // ny, 16, q), vb(nxc, nz, 16, q), vb(rows, q), vb(nxc, rows, q), vb(ny, rows, q),
        vb(ny, q, LANES), vb(ny, q, LANES), vb(ny, LANES, q), vf(nz * nxc, LANES), vf(nz, nxc, LANES),
        vb(width, width), vb(HEAD * HEAD, LANES), vb(rows, heads, HEAD * HEAD), vf(5, rows * heads, LANES),
        vb(rows * heads, HEAD * HEAD),
        vb(ny, nxc, 3, rows, LANES), vb(ny, 3, rows, width), vb(rows, q),
        vb(nz // 8, rows, width), vb(ny, nz // 8, rows, width), vb(ny, rows, q), vb(ny, rows, q),
        vb(nz, rows, q), vb(ny * q, LANES), vb(ny * q, LANES), vb(LANES, ny * q), vb(ny, rows, q), vb(ny, rows, q),
        vb(2, count, half * rows), vb(2, count, half * rows), vb(2, nxc, slots, q), vb(2, nxc, slots, q),
        vb(2, ny, count, 2 * LANES), vb(2, ny, count, 2 * LANES), vb(2, count, LANES), vb(2, ny, count, LANES),
        vb(2, nxc, slots, q), vb(2, nxc, slots, q), vb(nz, rows, q), vb(nz, rows, q),
        vb(2, nz // 4 - 1, rows, q), vb(rows, q), vb(2, rows, q),
        dma((300,)), dma((2, half, 6)), dma((nx, nz)), dma((nx,)), dma((nxc,)), dma((ny,)), dma((ny,)), dma((ny,)),
        dma((ny,)), dma((nz,)), dma((nxc * ny,)), dma((ny,)), dma((nz,)), dma((ny,)), dma((2, nxc)), dma((2, ny)),
        dma((2, ny)), dma((2, nxc)), dma((nz,)), dma((2, nz // 4 - 1)), dma, dma((21,)),
    ]
    return pl.pallas_call(
        functools.partial(layer, sizes),
        out_shape=jax.ShapeDtypeStruct((rows, q), BF16),
        in_specs=[hbm] * 21,
        out_specs=vmem,
        scratch_shapes=scratch,
        compiler_params=pltpu.CompilerParams(
            collective_id=0, has_side_effects=True
        ),
        name="layer",
    )(
        tokens, *turned, state, *line, routes.T, route_weight.T,
        expert_gate[0], expert_up[0], expert_down[0], shared_gate, shared_up, shared_down,
    )


def solution(mesh):
    shape = SHAPE if SHAPE else (16, 4, 2, mesh.shape["tp"])
    torus = Mesh(mesh.devices.reshape(shape), AXES)
    placed = (
        P(EP, "tp"), P(EP, "tp", None), P("tp"),
        P("tp", EP), P("tp", EP), P("tp", EP), P("tp", EP), P("tp", EP),
        P("tp"), P("tp"), P("tp"), P("tp", EP), P(), P(EP, None), P(EP, None),
        P(EP, None, "tp"), P(EP, None, "tp"), P(EP, "tp", None), P(None, "tp"), P(None, "tp"), P("tp", None),
    )
    return jax.shard_map(body, mesh=torus, in_specs=placed, out_specs=P(EP, "tp"), check_vma=False)


SHAPE = None
```
